256 devices in a mesh: tp: 32 (over z, x), dp: 8 (over y, core).
Axes of the slice: x: 4, y: 4, z: 8, core: 2. Of those that a mesh axis runs over, the one named last changes fastest.
Arguments:
- stream: bfloat16 [256, 4096], P(None, 'dp'), may hold values from -12 to 12
- history: int32 [256], P('dp'), may hold values from 1 to 4096, 262144 in all
- input_norm_gain: float32 [2, 4096], P(None, 'dp'), may hold values from 0.1 to 1.9
- query_weight: bfloat16 [2, 4096, 4096], P(None, 'dp', 'tp'), may hold values from -0.09375 to 0.09375
- key_weight: bfloat16 [2, 4096, 4096], P(None, 'dp', 'tp'), may hold values from -0.09375 to 0.09375
- value_weight: bfloat16 [2, 4096, 4096], P(None, 'dp', 'tp'), may hold values from -0.09375 to 0.09375
- gate_weight: bfloat16 [2, 4096, 4096], P(None, 'dp', 'tp'), may hold values from -0.09375 to 0.09375
- adapter_down_weight: bfloat16 [2, 4096, 128], P(None, 'dp'), may hold values from -0.09375 to 0.09375
- decay_up_weight: float32 [2, 64, 4096], P(None, None, 'tp'), may hold values from -3 to 3
- rate_up_weight: float32 [2, 64, 4096], P(None, None, 'tp'), may hold values from -3 to 3
- decay_offset: float32 [2, 4096], P(None, 'tp'), may hold values from -3 to 1
- head_norm_gain: float32 [2, 4096], P(None, 'tp'), may hold values from 0.1 to 1.9
- output_weight: bfloat16 [2, 4096, 4096], P(None, 'tp', 'dp'), may hold values from -0.09375 to 0.09375
- recurrent_state: float32 [2, 256, 64, 4096], P(None, 'dp', 'tp'), may hold values from -5 to 5
Outputs:
- stream_out: bfloat16 [256, 4096], P(None, 'dp')
- state_out: float32 [2, 256, 64, 4096], P(None, 'dp', 'tp')
The draws below stay inside these ranges and needn't reach their ends.
All inputs are finite; a program needn't handle non-finite values. No bound on the sum of `history` on one device may be relied on, other than what follows from the above.
Results may differ from the reference program's by a relative error of at most 0.024.
Values may be sent and summed in bfloat16 or wider, within the bound.
A program may use at most 64 MiB of HBM per device.

```python
import math
import jax
import jax.numpy as jnp
import numpy as np
from jax import lax

MODEL_WIDTH = 4096
HEAD = 64
ADAPTER_RANK = 64
SPAN = 64
BLOCK_COUNT = 2
BATCH = 256
HEADS = 64
N_DP = 8


def draw_stream(key, part):
    first_key, second_key = jax.random.split(jax.random.fold_in(key, 11))
    blocks = 8
    base = jax.random.normal(first_key, (BATCH, MODEL_WIDTH), jnp.float32)
    scales = jnp.exp(jax.random.uniform(second_key, (blocks,), jnp.float32, -1.1, 1.1))
    scales = jnp.repeat(scales, MODEL_WIDTH // blocks)
    return jnp.clip(base * scales[None, :], -12.0, 12.0).astype(jnp.bfloat16)


def level_of(own_key, extent, cuts, low, high):
    def one(position, shards_of):
        draws = jax.random.uniform(jax.random.fold_in(jax.random.fold_in(own_key, 6), position), (shards_of,), jnp.float32, low / len(cuts), high / len(cuts))
        return jnp.repeat(jnp.exp(draws), extent[position] // shards_of).reshape((-1,) + (1,) * (len(extent) - position - 1))

    loudness = one(*cuts[0])
    for cut in cuts[1:]:
        loudness = loudness * one(*cut)
    return loudness


def length_profile(count, total, limit, lean):
    loads = [(1 << 20) // math.isqrt(grade ** lean) + 1 for grade in range(2, count + 1)]
    spare, counts = total - limit - (count - 1), [1] * (count - 1)
    while spare > 0:
        candidates = [i for i in range(count - 1) if counts[i] < limit]
        mass, remaining = sum([loads[i] for i in candidates]), spare
        for i in candidates:
            more = min(limit - counts[i], max(1, remaining * loads[i] // mass), spare)
            counts[i] = counts[i] + more
            spare = spare - more
    return np.array([limit] + counts)


def ragged_sizes(stream_key, count, total, reach, slope):
    if count == 2:
        one = jax.random.randint(stream_key, (), max(1, total - reach), min(reach, total - 1) + 1)
        return jnp.stack([one, total - one])
    lengths = jnp.asarray(length_profile(count, total, reach, slope), jnp.int32)
    pairs = (count - 1) // 2
    donor, taker = lengths[1:1 + 2 * pairs:2], lengths[2:2 + 2 * pairs:2]
    room = jnp.minimum(donor - 1, reach - taker)
    shifted = jax.random.randint(jax.random.fold_in(stream_key, 1), (pairs,), 0, 1 << 20) % (room + 1)
    lengths = lengths.at[1:1 + 2 * pairs:2].set(donor - shifted).at[2:2 + 2 * pairs:2].set(taker + shifted)
    return lengths[jax.random.permutation(jax.random.fold_in(stream_key, 2), count)]


def gaussian(own_key, extent, scale, bound, pieces=(), dtype=jnp.bfloat16):
    entries = scale * jax.random.normal(own_key, extent, jnp.float32)
    if pieces:
        entries = entries * level_of(own_key, extent, pieces, -0.22, 0.18)
    return jnp.clip(entries, -bound, bound).astype(dtype)


def setup_inputs(seed: int = 0) -> dict:
    streams_of = jax.random.split(jax.random.key(seed), 15)
    stream = draw_stream(jax.random.fold_in(streams_of[14], 71), 0)
    history = ragged_sizes(streams_of[1], BATCH, 1024 * BATCH, 4096, 2).astype(jnp.int32)
    input_norm_gain = jnp.clip(1.0 + 0.18 * jax.random.normal(streams_of[2], (BLOCK_COUNT, MODEL_WIDTH), jnp.float32), 0.1, 1.9)
    query_weight = gaussian(streams_of[3], (BLOCK_COUNT, MODEL_WIDTH, MODEL_WIDTH), MODEL_WIDTH ** -0.5, 0.09375, ((1, 8), (2, 32)))
    key_weight = gaussian(streams_of[4], (BLOCK_COUNT, MODEL_WIDTH, MODEL_WIDTH), MODEL_WIDTH ** -0.5, 0.09375, ((1, 8), (2, 32)))
    value_weight = gaussian(streams_of[5], (BLOCK_COUNT, MODEL_WIDTH, MODEL_WIDTH), MODEL_WIDTH ** -0.5, 0.09375, ((1, 8), (2, 32)))
    gate_weight = gaussian(streams_of[6], (BLOCK_COUNT, MODEL_WIDTH, MODEL_WIDTH), MODEL_WIDTH ** -0.5, 0.09375, ((1, 8), (2, 32)))
    adapter_down_weight = gaussian(streams_of[7], (BLOCK_COUNT, MODEL_WIDTH, 2 * ADAPTER_RANK), MODEL_WIDTH ** -0.5, 0.09375, ((1, 8),))
    decay_up_weight = gaussian(streams_of[8], (BLOCK_COUNT, ADAPTER_RANK, MODEL_WIDTH), (ADAPTER_RANK // 16) ** -0.5, 3.0, ((2, 32),), jnp.float32)
    rate_up_weight = gaussian(streams_of[9], (BLOCK_COUNT, ADAPTER_RANK, MODEL_WIDTH), (ADAPTER_RANK // 16) ** -0.5, 3.0, ((2, 32),), jnp.float32)
    decay_offset = jnp.clip(-3.0 + 4.0 * jax.random.uniform(streams_of[10], (BLOCK_COUNT, MODEL_WIDTH), jnp.float32) ** level_of(streams_of[10], (BLOCK_COUNT, MODEL_WIDTH), ((1, 32),), -0.2, 0.2), -3.0, 1.0)
    head_norm_gain = jnp.clip(1.0 + 0.18 * jax.random.normal(streams_of[11], (BLOCK_COUNT, MODEL_WIDTH), jnp.float32), 0.1, 1.9)
    output_weight = gaussian(streams_of[12], (BLOCK_COUNT, MODEL_WIDTH, MODEL_WIDTH), MODEL_WIDTH ** -0.5, 0.09375, ((1, 32), (2, 8)))
    recurrent_state = gaussian(streams_of[13], (BLOCK_COUNT, BATCH, HEADS, HEAD * HEAD), 1.0, 5.0, ((1, 8), (2, 32)), jnp.float32)
    return {"stream": stream, "history": history, "input_norm_gain": input_norm_gain, "query_weight": query_weight, "key_weight": key_weight, "value_weight": value_weight, "gate_weight": gate_weight, "adapter_down_weight": adapter_down_weight, "decay_up_weight": decay_up_weight, "rate_up_weight": rate_up_weight, "decay_offset": decay_offset, "head_norm_gain": head_norm_gain, "output_weight": output_weight, "recurrent_state": recurrent_state}


NORM_EPS = 0.25
GROUP_EPS = 0.25

def projected_rows(rescaled_rows, weight):
    batch_rows = rescaled_rows.shape[0]
    blocked = rescaled_rows.reshape(batch_rows, N_DP, MODEL_WIDTH // N_DP).astype(jnp.float32)
    weight_blocks = weight.reshape(N_DP, MODEL_WIDTH // N_DP, weight.shape[1]).astype(jnp.float32)
    partials = jnp.einsum('bnd,ndc->nbc', blocked, weight_blocks)
    rounded = lax.optimization_barrier(partials.astype(jnp.bfloat16))
    return lax.optimization_barrier(jnp.sum(rounded.astype(jnp.float32), axis=0))

def mixing_block(stream, history, input_norm_gain, query_weight, key_weight, value_weight, gate_weight, adapter_down_weight, decay_up_weight, rate_up_weight, decay_offset, head_norm_gain, output_weight, recurrent_state):
    widened = stream.astype(jnp.float32)
    squares = lax.optimization_barrier(jnp.sum(widened * widened, axis=1))
    inverse_root_mean = lax.rsqrt(squares / MODEL_WIDTH + NORM_EPS)[:, None]
    rescaled_rows = (widened * input_norm_gain[None, :]).astype(jnp.bfloat16)
    query = projected_rows(rescaled_rows, query_weight) * inverse_root_mean
    key_proj = projected_rows(rescaled_rows, key_weight) * inverse_root_mean
    value_proj = projected_rows(rescaled_rows, value_weight) * inverse_root_mean
    gate_pre = projected_rows(rescaled_rows, gate_weight) * inverse_root_mean
    adapter_hidden = projected_rows(rescaled_rows, adapter_down_weight) * inverse_root_mean
    pos_factor = 0.5 + (history // SPAN % 3).astype(jnp.float32)
    decay_logits = decay_offset[None, :] + jnp.dot(jnp.tanh(adapter_hidden[:, :ADAPTER_RANK]), decay_up_weight, precision=lax.Precision.HIGHEST)
    rate_log = -jax.nn.softplus(-decay_logits) - 0.5
    decay = jnp.exp(-jnp.exp(rate_log) * pos_factor[:, None])
    learning_rate = jax.nn.sigmoid(jnp.dot(adapter_hidden[:, ADAPTER_RANK:], rate_up_weight, precision=lax.Precision.HIGHEST))
    batch_rows = widened.shape[0]
    head_count = MODEL_WIDTH // HEAD

    def heads_of(values):
        return values.reshape(batch_rows, head_count, HEAD)
    keys = heads_of(key_proj)
    key_unit = keys * lax.rsqrt(lax.optimization_barrier(jnp.sum(keys * keys, axis=-1, keepdims=True)) + 1.0)
    key_rate = key_unit * heads_of(learning_rate)
    matrix = recurrent_state.reshape(batch_rows, head_count, HEAD, HEAD)
    state_key = jnp.einsum('bhvk,bhk->bhv', matrix, key_unit)
    refreshed_state = matrix * heads_of(decay)[:, :, None, :] - state_key[..., None] * key_rate[:, :, None, :] + heads_of(value_proj)[..., None] * keys[:, :, None, :]
    readout = jnp.einsum('bhvk,bhk->bhv', refreshed_state, heads_of(query))
    mean_y = lax.optimization_barrier(jnp.mean(readout, axis=-1, keepdims=True))
    spread = lax.optimization_barrier(jnp.mean(jnp.square(readout - mean_y), axis=-1, keepdims=True))
    normed = ((readout - mean_y) * lax.rsqrt(spread + GROUP_EPS)).reshape(batch_rows, MODEL_WIDTH) * head_norm_gain[None, :]
    mixed = (normed * jax.nn.sigmoid(gate_pre)).astype(jnp.bfloat16)
    out_sum = jnp.dot(mixed, output_weight, preferred_element_type=jnp.float32)
    return ((widened + out_sum).astype(jnp.bfloat16), refreshed_state.reshape(batch_rows, head_count, HEAD * HEAD))

def reference(stream, history, input_norm_gain, query_weight, key_weight, value_weight, gate_weight, adapter_down_weight, decay_up_weight, rate_up_weight, decay_offset, head_norm_gain, output_weight, recurrent_state):
    new_states = []
    for layer_lookup in range(BLOCK_COUNT):
        stream, refreshed_state = mixing_block(stream, history, input_norm_gain[layer_lookup], query_weight[layer_lookup], key_weight[layer_lookup], value_weight[layer_lookup], gate_weight[layer_lookup], adapter_down_weight[layer_lookup], decay_up_weight[layer_lookup], rate_up_weight[layer_lookup], decay_offset[layer_lookup], head_norm_gain[layer_lookup], output_weight[layer_lookup], recurrent_state[layer_lookup])
        new_states.append(refreshed_state)
    return (stream, jnp.stack(new_states))
```

```python
import jax
import jax.numpy as jnp
from jax import lax
from jax.experimental import pallas as pl
from jax.experimental.pallas import tpu as pltpu
from jax.sharding import PartitionSpec as P

MODEL_WIDTH = 4096
HEAD = 64
ADAPTER_RANK = 64
SPAN = 64
BLOCKS = 2
NORM_EPS = 0.25
GROUP_EPS = 0.25

N_Y, N_CORE, N_Z, N_X = 4, 2, 8, 4
N_DP, N_TP = N_Y * N_CORE, N_Z * N_X
BATCH = 256
SEQS = BATCH // N_DP
ROWS = BATCH // N_TP
FEATS = MODEL_WIDTH // N_DP
WIDTH = MODEL_WIDTH // N_TP
PAIRS = SEQS * HEAD
WIDE = 4 * WIDTH + 2 * ADAPTER_RANK

F32, BF16 = jnp.float32, jnp.bfloat16
MESH = pl.DeviceIdType.MESH
EXACT = lax.Precision.HIGHEST

DP_STEPS = [(dy, dc) for dy in (2, 1, 3) for dc in (0, 1)] + [(0, 1)]
TP_STEPS = sorted(
    [(dz, dx) for dz in range(N_Z) for dx in range(N_X) if (dz, dx) != (0, 0)],
    key=lambda s: -(min(s[0], N_Z - s[0]) + min(s[1], N_X - s[1])),
)


def stable_sigmoid(x):
    e = jnp.exp(-jnp.abs(x))
    return jnp.where(x >= 0, 1.0, e) / (1.0 + e)


def iota(shape, dim):
    return lax.broadcasted_iota(jnp.int32, shape, dim)


def kernel(
    hist, gain, decay_off, head_gain, stream_in,
    qw, kw, vw, gw, aw, du, ru, ow, state_in,
    stream_out, state_out,
    w_all, w_low, w_out, state, part, part_in, sq, sq_in, mixed, mixed_in, osum, osum_in, rows, stream_mid,
    load_sem, state_sem, send_sem, recv_sem,
):
    me_t, me_d = lax.axis_index("tp"), lax.axis_index("dp")
    z, x = me_t // N_X, me_t % N_X
    y, core = me_d // N_CORE, me_d % N_CORE
    dp_peers = [((y + dy) % N_Y) * N_CORE + (core + dc) % N_CORE for dy, dc in DP_STEPS]
    tp_peers = [((z + dz) % N_Z) * N_X + (x + dx) % N_X for dz, dx in TP_STEPS]

    barrier = pltpu.get_barrier_semaphore()
    for p in tp_peers:
        pl.semaphore_signal(barrier, inc=1, device_id={"tp": p}, device_id_type=MESH)
    for p in dp_peers:
        pl.semaphore_signal(barrier, inc=1, device_id={"dp": p}, device_id_type=MESH)

    loads = []
    for l in range(BLOCKS):
        pairs = [
            (w.at[l], w_all.at[l, :, pl.ds(i * WIDTH, WIDTH)]) for i, w in enumerate((qw, kw, vw, gw, aw))
        ]
        pairs += [
            (du.at[l], w_low.at[l, pl.ds(0, 64), pl.ds(0, WIDTH)]),
            (ru.at[l], w_low.at[l, pl.ds(64, 64), pl.ds(WIDTH, WIDTH)]),
            (ow.at[l], w_out.at[l]),
            (state_in.at[l], state.at[l]),
        ]
        loads.append([pltpu.make_async_copy(s, d, load_sem.at[l, i]) for i, (s, d) in enumerate(pairs)])
    for c in loads[0]:
        c.start()
    for c in loads[1]:
        c.start()
    for l in range(BLOCKS):
        w_low[l, pl.ds(0, 64), pl.ds(WIDTH, WIDTH)] = jnp.zeros((64, WIDTH), F32)
        w_low[l, pl.ds(64, 64), pl.ds(0, WIDTH)] = jnp.zeros((64, WIDTH), F32)

    low_lane = iota((SEQS, WIDTH), 1) < HEAD
    seg = ((iota((WIDTH, WIDTH), 0) // HEAD) == (iota((WIDTH, WIDTH), 1) // HEAD)).astype(F32)
    fold = ((iota((WIDTH, WIDTH), 0) // HEAD) == (iota((WIDTH, WIDTH), 1) % 2)).astype(F32).astype(BF16)
    spread = ((iota((WIDTH, WIDTH), 1) // HEAD) == (iota((WIDTH, WIDTH), 0) % 2)).astype(F32).astype(BF16)
    r_i, l_i = iota((HEAD, WIDTH), 0), iota((HEAD, WIDTH), 1)
    pick = ((l_i // HEAD == r_i % 2) & ((l_i % HEAD) // 2 == r_i // 2)).astype(F32)
    even_row = (iota((SEQS, 8, WIDTH), 1) % 2) == 0
    eye = iota((128, 128), 0) == iota((128, 128), 1)
    mine = iota((SEQS, BATCH), 1) == iota((SEQS, BATCH), 0) + me_d * SEQS

    pos = jnp.zeros((SEQS, WIDTH), F32)
    seq_i = iota((SEQS, WIDTH), 0)
    for i in range(SEQS):
        pos = jnp.where(seq_i == i, 0.5 + ((hist[i] // SPAN) % 3).astype(F32), pos)

    def per_row(v):
        r = pltpu.roll(v, HEAD, 1)
        t0, t1 = jnp.where(low_lane, v, r), jnp.where(low_lane, r, v)
        return jnp.where(even_row, t0[:, None, :], t1[:, None, :])

    def split_dot(v, m):
        hi = v.astype(BF16)
        lo = (v - hi.astype(F32)).astype(BF16)
        return jnp.dot(hi, m, preferred_element_type=F32) + jnp.dot(lo, m, preferred_element_type=F32)

    def send(src, dst, l, s, peer):
        pltpu.make_async_remote_copy(
            src_ref=src, dst_ref=dst, send_sem=send_sem.at[l, s], recv_sem=recv_sem.at[l, s],
            device_id=peer, device_id_type=MESH,
        ).start()

    def wait_bytes(ref, sem):
        pltpu.make_async_copy(ref, ref, sem).wait()

    for l in range(BLOCKS):
        stream = stream_in if l == 0 else stream_mid.at[l - 1]
        xf = stream[...].astype(F32).reshape(BATCH, FEATS)
        sq_col = jnp.sum(xf * xf, axis=1, keepdims=True)
        for i in range(BATCH // 128):
            sq[l, :, pl.ds(i * 128, 128)] = jnp.sum(
                jnp.where(eye, sq_col[i * 128 : (i + 1) * 128], 0.0), axis=0, keepdims=True
            )
        scaled = (xf * gain[pl.ds(l, 1), :]).astype(BF16)
        for c in loads[l][:5]:
            c.wait()
        product = jnp.dot(scaled, w_all[l], preferred_element_type=F32)
        part[l] = product.astype(BF16).reshape(N_DP, SEQS, WIDE)
        if l == 0:
            pl.semaphore_wait(barrier, len(tp_peers) + len(dp_peers))
        for p in dp_peers:
            send(part.at[l, p], part_in.at[l, me_d], l, 0, {"dp": p})
        for p in dp_peers:
            send(sq.at[l], sq_in.at[l, me_d], l, 1, {"dp": p})
        part_in[l, me_d] = part[l, me_d]
        sq_in[l, me_d] = sq[l]
        for c in loads[l][5:]:
            c.wait()

        wait_bytes(sq_in.at[l, pl.ds(0, N_DP - 1)], recv_sem.at[l, 1])
        sq_all = sq_in[l, 0]
        for d in range(1, N_DP):
            sq_all = sq_all + sq_in[l, d]
        own_sq = jnp.sum(jnp.where(mine, sq_all, 0.0), axis=1, keepdims=True)
        inv = lax.rsqrt(own_sq / MODEL_WIDTH + NORM_EPS)
        wait_bytes(part_in.at[l, pl.ds(0, N_DP - 1)], recv_sem.at[l, 0])
        total = part_in[l, 0].astype(F32)
        for d in range(1, N_DP):
            total = total + part_in[l, d].astype(F32)
        total = total * inv
        query, key, value, gate, low = [total[:, i * WIDTH : (i + 1) * WIDTH] for i in range(5)]

        low = jnp.where(low_lane, jnp.tanh(low), low)
        up = jnp.dot(low, w_low[l], preferred_element_type=F32, precision=EXACT)
        decay = jnp.exp(
            -(stable_sigmoid(decay_off[pl.ds(l, 1), :] + up[:, :WIDTH]) * 0.6065306597126334) * pos
        )
        learn = stable_sigmoid(up[:, WIDTH:])
        sums = jnp.dot(
            jnp.concatenate([key * key, key * learn * query, key * query], axis=0), seg,
            preferred_element_type=F32, precision=EXACT,
        )
        key_inv = lax.rsqrt(sums[:SEQS] + 1.0)
        key_unit = key * key_inv
        key_rate = key_unit * learn
        rate_query, key_query = sums[SEQS : 2 * SEQS] * key_inv, sums[2 * SEQS :]

        unit_rows, query_rows = per_row(key_unit), per_row(decay * query)
        got = []
        for rows8 in (unit_rows, query_rows):
            prod = state[l].reshape(SEQS, HEAD // 8, 8, WIDTH) * rows8[:, None]
            folded = split_dot(prod.reshape(PAIRS, WIDTH), fold).reshape(SEQS, HEAD, WIDTH)
            got.append(jnp.sum(folded * pick[None], axis=1))
        state_key, state_query = got
        readout = state_query - state_key * rate_query + value * key_query
        mean = jnp.dot(readout, seg, preferred_element_type=F32, precision=EXACT) * (1.0 / HEAD)
        centred = readout - mean
        var = jnp.dot(centred * centred, seg, preferred_element_type=F32, precision=EXACT) * (1.0 / HEAD)
        normed = centred * lax.rsqrt(var + GROUP_EPS) * head_gain[pl.ds(l, 1), :]
        own_mixed = (normed * stable_sigmoid(gate)).astype(BF16)
        mixed[l] = own_mixed
        for p in dp_peers:
            send(mixed.at[l], mixed_in.at[l, me_d], l, 2, {"dp": p})
        mixed_in[l, me_d] = own_mixed

        def outer(v):
            return split_dot((v[:, None, :] * pick[None]).reshape(PAIRS, WIDTH), spread).reshape(
                SEQS, HEAD // 8, 8, WIDTH
            )

        state[l] = (
            state[l].reshape(SEQS, HEAD // 8, 8, WIDTH) * per_row(decay)[:, None]
            - outer(state_key) * per_row(key_rate)[:, None]
            + outer(value) * per_row(key)[:, None]
        ).reshape(PAIRS, WIDTH)
        pltpu.make_async_copy(state.at[l], state_out.at[l], state_sem.at[l]).start()

        wait_bytes(mixed_in.at[l, pl.ds(0, N_DP - 1)], recv_sem.at[l, 2])
        out_part = jnp.dot(mixed_in[l].reshape(BATCH, WIDTH), w_out[l], preferred_element_type=F32)
        osum[l] = out_part.reshape(N_TP, ROWS, FEATS).astype(BF16)
        for p in tp_peers:
            send(osum.at[l, p], osum_in.at[l, me_t], l, 3, {"tp": p})
        osum_in[l, me_t] = osum[l, me_t]
        wait_bytes(osum_in.at[l, pl.ds(0, N_TP - 1)], recv_sem.at[l, 3])
        new = stream[me_t].astype(F32) + jnp.sum(osum_in[l].astype(F32), axis=0)
        rows[l] = new.astype(BF16)
        for p in tp_peers:
            send(rows.at[l], stream_mid.at[l, me_t], l, 4, {"tp": p})
        stream_mid[l, me_t] = rows[l]
        wait_bytes(stream_mid.at[l, pl.ds(0, N_TP - 1)], recv_sem.at[l, 4])

    stream_out[...] = stream_mid[BLOCKS - 1]
    for l in range(BLOCKS):
        pltpu.make_async_copy(state.at[l], state_out.at[l], state_sem.at[l]).wait()
        wait_bytes(part.at[l, pl.ds(0, N_DP - 1)], send_sem.at[l, 0])
        wait_bytes(sq_in.at[l, pl.ds(0, N_DP - 1)], send_sem.at[l, 1])
        wait_bytes(mixed_in.at[l, pl.ds(0, N_DP - 1)], send_sem.at[l, 2])
        wait_bytes(osum.at[l, pl.ds(0, N_TP - 1)], send_sem.at[l, 3])
        wait_bytes(stream_mid.at[l, pl.ds(0, N_TP - 1)], send_sem.at[l, 4])


def body(
    stream, history, input_norm_gain, query_weight, key_weight, value_weight, gate_weight, adapter_down_weight,
    decay_up_weight, rate_up_weight, decay_offset, head_norm_gain, output_weight, recurrent_state,
):
    state = recurrent_state.reshape(BLOCKS, SEQS, 2, HEAD // 2, WIDTH).transpose(0, 1, 3, 2, 4)
    state = state.reshape(BLOCKS, PAIRS, WIDTH)
    vmem, anywhere = pl.BlockSpec(memory_space=pltpu.VMEM), pl.BlockSpec(memory_space=pl.ANY)
    new_stream, new_state = pl.pallas_call(
        kernel,
        out_shape=(
            jax.ShapeDtypeStruct((N_TP, ROWS, FEATS), BF16),
            jax.ShapeDtypeStruct((BLOCKS, PAIRS, WIDTH), F32),
        ),
        in_specs=[pl.BlockSpec(memory_space=pltpu.SMEM), vmem, vmem, vmem, vmem] + [anywhere] * 9,
        out_specs=(vmem, anywhere),
        scratch_shapes=[
            pltpu.VMEM((BLOCKS, FEATS, WIDE), BF16),
            pltpu.VMEM((BLOCKS, 2 * ADAPTER_RANK, 2 * WIDTH), F32),
            pltpu.VMEM((BLOCKS, WIDTH, FEATS), BF16),
            pltpu.VMEM((BLOCKS, PAIRS, WIDTH), F32),
            pltpu.VMEM((BLOCKS, N_DP, SEQS, WIDE), BF16),
            pltpu.VMEM((BLOCKS, N_DP, SEQS, WIDE), BF16),
            pltpu.VMEM((BLOCKS, 1, BATCH), F32),
            pltpu.VMEM((BLOCKS, N_DP, 1, BATCH), F32),
            pltpu.VMEM((BLOCKS, SEQS, WIDTH), BF16),
            pltpu.VMEM((BLOCKS, N_DP, SEQS, WIDTH), BF16),
            pltpu.VMEM((BLOCKS, N_TP, ROWS, FEATS), BF16),
            pltpu.VMEM((BLOCKS, N_TP, ROWS, FEATS), BF16),
            pltpu.VMEM((BLOCKS, ROWS, FEATS), BF16),
            pltpu.VMEM((BLOCKS, N_TP, ROWS, FEATS), BF16),
            pltpu.SemaphoreType.DMA((BLOCKS, 9)),
            pltpu.SemaphoreType.DMA((BLOCKS,)),
            pltpu.SemaphoreType.DMA((BLOCKS, 5)),
            pltpu.SemaphoreType.DMA((BLOCKS, 5)),
        ],
        compiler_params=pltpu.CompilerParams(collective_id=0, has_side_effects=True),
        name="two_blocks",
    )(
        history, input_norm_gain, decay_offset, head_norm_gain, stream.reshape(N_TP, ROWS, FEATS),
        query_weight, key_weight, value_weight, gate_weight, adapter_down_weight,
        decay_up_weight, rate_up_weight, output_weight, state,
    )
    new_state = new_state.reshape(BLOCKS, SEQS, HEAD // 2, 2, WIDTH).transpose(0, 1, 3, 2, 4)
    return new_stream.reshape(BATCH, FEATS), new_state.reshape(BLOCKS, SEQS, 2, HEAD * HEAD)


def solution(mesh):
    placed = (
        P(None, "dp"), P("dp"), P(None, "dp"),
        P(None, "dp", "tp"), P(None, "dp", "tp"), P(None, "dp", "tp"), P(None, "dp", "tp"),
        P(None, "dp", None), P(None, None, "tp"), P(None, None, "tp"), P(None, "tp"), P(None, "tp"),
        P(None, "tp", "dp"), P(None, "dp", "tp", None),
    )
    return jax.shard_map(
        body,
        mesh=mesh,
        in_specs=placed,
        out_specs=(P(None, "dp"), P(None, "dp", "tp", None)),
        check_vma=False,
    )
```

```python
import jax
import jax.numpy as jnp
from jax import lax
from jax.experimental import pallas as pl
from jax.experimental.pallas import tpu as pltpu
from jax.sharding import PartitionSpec as P

MODEL_WIDTH = 4096
HEAD = 64
ADAPTER_RANK = 64
SPAN = 64
BLOCKS = 2
NORM_EPS = 0.25
GROUP_EPS = 0.25

N_Y, N_CORE, N_Z, N_X = 4, 2, 8, 4
N_DP, N_TP = N_Y * N_CORE, N_Z * N_X
BATCH = 256
SEQS = BATCH // N_DP
ROWS = BATCH // N_TP
FEATS = MODEL_WIDTH // N_DP
WIDTH = MODEL_WIDTH // N_TP
PAIRS = SEQS * HEAD
WIDE = 4 * WIDTH + 2 * ADAPTER_RANK

F32, BF16 = jnp.float32, jnp.bfloat16
MESH = pl.DeviceIdType.MESH
EXACT = lax.Precision.HIGHEST

def hops(step, size):
    return min(step, size - step)


DP_STEPS = [(dy, dc) for dy in (2, 1, 3) for dc in (0, 1)] + [(0, 1)]
Z_STEPS = [4, 3, 5, 2, 6, 1, 7]
X_STEPS = [2, 1, 3]
SLAB_STEPS = sorted(
    [(dx, dy, dc) for dx in range(N_X) for dy in range(N_Y) for dc in range(N_CORE) if (dx, dy, dc) != (0, 0, 0)],
    key=lambda s: -(hops(s[0], N_X) + hops(s[1], N_Y)),
)


def stable_sigmoid(x):
    e = jnp.exp(-jnp.abs(x))
    return jnp.where(x >= 0, 1.0, e) / (1.0 + e)


def iota(shape, dim):
    return lax.broadcasted_iota(jnp.int32, shape, dim)


def kernel(
    hist_in, gain_in, decay_off_in, head_gain_in, stream_in, qw, kw, vw, gw, aw, du, ru, ow, state_in,
    stream_out, state_out,
    hist, gain, decay_off, head_gain, first, w_all, w_low, w_out, state,
    part, part_in, sq, sq_in, mixed, mixed_in, osum, osum_in, rows, stream_mid,
    load_sem, misc_sem, send_sem, recv_sem, ring_sem,
):
    me_t, me_d = lax.axis_index("tp"), lax.axis_index("dp")
    z, x = me_t // N_X, me_t % N_X
    y, core = me_d // N_CORE, me_d % N_CORE
    dp_peers = [((y + dy) % N_Y) * N_CORE + (core + dc) % N_CORE for dy, dc in DP_STEPS]
    z_peers = [(dz, (z + dz) % N_Z) for dz in Z_STEPS]
    x_peers = [(x + dx) % N_X for dx in X_STEPS]
    slab_peers = [
        ((x + dx) % N_X, ((y + dy) % N_Y) * N_CORE + (core + dc) % N_CORE) for dx, dy, dc in SLAB_STEPS
    ]

    barrier = pltpu.get_barrier_semaphore()
    for px, pd in slab_peers:
        pl.semaphore_signal(barrier, inc=1, device_id={"tp": z * N_X + px, "dp": pd}, device_id_type=MESH)
    for _, p in z_peers:
        pl.semaphore_signal(barrier, inc=1, device_id={"tp": p * N_X + x}, device_id_type=MESH)

    def start(src, dst, sem):
        c = pltpu.make_async_copy(src, dst, sem)
        c.start()
        return c

    first_loads = [start(stream_in, first, misc_sem.at[0]), start(gain_in, gain, misc_sem.at[1])]
    weight_loads, small_loads, state_loads = [], [], []
    for l in range(BLOCKS):
        weight_loads.append([
            start(w.at[l], w_all.at[l, :, pl.ds(i * WIDTH, WIDTH)], load_sem.at[l, i])
            for i, w in enumerate((qw, kw, vw, gw, aw))
        ])
        small_loads.append([
            start(du.at[l], w_low.at[l, pl.ds(0, 64), pl.ds(0, WIDTH)], load_sem.at[l, 5]),
            start(ru.at[l], w_low.at[l, pl.ds(64, 64), pl.ds(WIDTH, WIDTH)], load_sem.at[l, 6]),
            start(ow.at[l], w_out.at[l, x], load_sem.at[l, 7]),
        ])
        if l == 0:
            small_loads[0] += [
                start(hist_in, hist, misc_sem.at[2]),
                start(decay_off_in, decay_off, misc_sem.at[3]),
                start(head_gain_in, head_gain, misc_sem.at[4]),
            ]
        state_loads.append(start(state_in.at[l], state.at[l], load_sem.at[l, 8]))

    def send(src, dst, l, s, peer, sem=None):
        pltpu.make_async_remote_copy(
            src_ref=src, dst_ref=dst, send_sem=send_sem.at[l, s],
            recv_sem=recv_sem.at[l, s] if sem is None else sem,
            device_id=peer, device_id_type=MESH,
        ).start()

    def wait_bytes(ref, sem):
        pltpu.make_async_copy(ref, ref, sem).wait()

    def per_row(v):
        r = pltpu.roll(v, HEAD, 1)
        t0, t1 = jnp.where(low_lane, v, r), jnp.where(low_lane, r, v)
        return jnp.where(even_row, t0[:, None, :], t1[:, None, :])

    def split_dot(v, m):
        hi = v.astype(BF16)
        lo = (v - hi.astype(F32)).astype(BF16)
        return jnp.dot(hi, m, preferred_element_type=F32) + jnp.dot(lo, m, preferred_element_type=F32)

    eye = iota((128, 128), 0) == iota((128, 128), 1)
    for l in range(BLOCKS):
        with jax.named_scope("project"):
            if l == 0:
                for c in first_loads:
                    c.wait()
            stream = first if l == 0 else stream_mid
            xf = stream[...].astype(F32).reshape(BATCH, FEATS)
            sq_col = jnp.sum(xf * xf, axis=1, keepdims=True)
            for i in range(BATCH // 128):
                sq[l, :, pl.ds(i * 128, 128)] = jnp.sum(
                    jnp.where(eye, sq_col[i * 128 : (i + 1) * 128], 0.0), axis=0, keepdims=True
                )
            scaled = (xf * gain[pl.ds(l, 1), :]).astype(BF16)
            for c in weight_loads[l]:
                c.wait()
            product = jnp.dot(scaled, w_all[l], preferred_element_type=F32)
            part[l] = product.astype(BF16).reshape(N_DP, SEQS, WIDE)
        with jax.named_scope("barrier"):
            if l == 0:
                pl.semaphore_wait(barrier, len(slab_peers) + len(z_peers))
        with jax.named_scope("send_part"):
            for p in dp_peers:
                send(part.at[l, p], part_in.at[l, me_d], l, 0, {"dp": p})
            for p in dp_peers:
                send(sq.at[l], sq_in.at[l, me_d], l, 1, {"dp": p})
            part_in[l, me_d] = part[l, me_d]
            sq_in[l, me_d] = sq[l]
            for p in x_peers:
                send(ow.at[l], w_out.at[l, x], l, 5, {"tp": z * N_X + p})
            for c in small_loads[l]:
                c.wait()
            w_low[l, pl.ds(0, 64), pl.ds(WIDTH, WIDTH)] = jnp.zeros((64, WIDTH), F32)
            w_low[l, pl.ds(64, 64), pl.ds(0, WIDTH)] = jnp.zeros((64, WIDTH), F32)
            if l == 0:
                low_lane = iota((SEQS, WIDTH), 1) < HEAD
                seg = ((iota((WIDTH, WIDTH), 0) // HEAD) == (iota((WIDTH, WIDTH), 1) // HEAD)).astype(F32)
                half, parity = iota((WIDTH, WIDTH), 0) // HEAD, iota((WIDTH, WIDTH), 1) % 2
                fold = (half == parity).astype(F32).astype(BF16)
                half, parity = iota((WIDTH, WIDTH), 1) // HEAD, iota((WIDTH, WIDTH), 0) % 2
                spread = (half == parity).astype(F32).astype(BF16)
                r_i, l_i = iota((HEAD, WIDTH), 0), iota((HEAD, WIDTH), 1)
                pick = ((l_i // HEAD == r_i % 2) & ((l_i % HEAD) // 2 == r_i // 2)).astype(F32)
                even_row = (iota((SEQS, 8, WIDTH), 1) % 2) == 0
                mine = iota((SEQS, BATCH), 1) == iota((SEQS, BATCH), 0) + me_d * SEQS
                pos = jnp.zeros((SEQS, WIDTH), F32)
                seq_i = iota((SEQS, WIDTH), 0)
                for i in range(SEQS):
                    pos = jnp.where(seq_i == i, 0.5 + ((hist[i] // SPAN) % 3).astype(F32), pos)
            state_loads[l].wait()
        with jax.named_scope("wait_part"):
            wait_bytes(sq_in.at[l, pl.ds(0, N_DP - 1)], recv_sem.at[l, 1])
            sq_all = sq_in[l, 0]
            for d in range(1, N_DP):
                sq_all = sq_all + sq_in[l, d]
            own_sq = jnp.sum(jnp.where(mine, sq_all, 0.0), axis=1, keepdims=True)
            inv = lax.rsqrt(own_sq / MODEL_WIDTH + NORM_EPS)
            wait_bytes(part_in.at[l, pl.ds(0, N_DP - 1)], recv_sem.at[l, 0])
        with jax.named_scope("recur"):
            total = part_in[l, 0].astype(F32)
            for d in range(1, N_DP):
                total = total + part_in[l, d].astype(F32)
            total = total * inv
            query, key, value, gate, low = [total[:, i * WIDTH : (i + 1) * WIDTH] for i in range(5)]

            low = jnp.where(low_lane, jnp.tanh(low), low)
            up = jnp.dot(low, w_low[l], preferred_element_type=F32, precision=EXACT)
            decay = jnp.exp(
                -(stable_sigmoid(decay_off[pl.ds(l, 1), :] + up[:, :WIDTH]) * 0.6065306597126334) * pos
            )
            learn = stable_sigmoid(up[:, WIDTH:])
            sums = jnp.dot(
                jnp.concatenate([key * key, key * learn * query, key * query], axis=0), seg,
                preferred_element_type=F32, precision=EXACT,
            )
            key_inv = lax.rsqrt(sums[:SEQS] + 1.0)
            key_unit = key * key_inv
            key_rate = key_unit * learn
            rate_query, key_query = sums[SEQS : 2 * SEQS] * key_inv, sums[2 * SEQS :]

            unit_rows, query_rows = per_row(key_unit), per_row(decay * query)
            got = []
            for rows8 in (unit_rows, query_rows):
                prod = state[l].reshape(SEQS, HEAD // 8, 8, WIDTH) * rows8[:, None]
                folded = split_dot(prod.reshape(PAIRS, WIDTH), fold).reshape(SEQS, HEAD, WIDTH)
                got.append(jnp.sum(folded * pick[None], axis=1))
            state_key, state_query = got
            readout = state_query - state_key * rate_query + value * key_query
            mean = jnp.dot(readout, seg, preferred_element_type=F32, precision=EXACT) * (1.0 / HEAD)
            centred = readout - mean
            var = jnp.dot(centred * centred, seg, preferred_element_type=F32, precision=EXACT) * (1.0 / HEAD)
            normed = centred * lax.rsqrt(var + GROUP_EPS) * head_gain[pl.ds(l, 1), :]
            own_mixed = (normed * stable_sigmoid(gate)).astype(BF16)
        with jax.named_scope("send_mixed"):
            own_mixed = own_mixed.reshape(N_X, ROWS, WIDTH)
            mixed[l] = own_mixed
            for px, pd in slab_peers:
                send(mixed.at[l, px], mixed_in.at[l, x * N_DP + me_d], l, 2, {"tp": z * N_X + px, "dp": pd})
            mixed_in[l, x * N_DP + me_d] = mixed[l, x]
        with jax.named_scope("update"):

            def outer(v):
                return split_dot((v[:, None, :] * pick[None]).reshape(PAIRS, WIDTH), spread).reshape(
                    SEQS, HEAD // 8, 8, WIDTH
                )

            state_out[l] = (
                state[l].reshape(SEQS, HEAD // 8, 8, WIDTH) * per_row(decay)[:, None]
                - outer(state_key) * per_row(key_rate)[:, None]
                + outer(value) * per_row(key)[:, None]
            ).reshape(PAIRS, WIDTH)
        with jax.named_scope("wait_mixed"):
            wait_bytes(w_out.at[l, pl.ds(0, N_X - 1)], recv_sem.at[l, 5])
            wait_bytes(mixed_in.at[l, pl.ds(0, len(slab_peers))], recv_sem.at[l, 2])
        with jax.named_scope("output"):
            out_part = jnp.zeros((N_DP * ROWS, FEATS), F32)
            for i in range(N_X):
                out_part = out_part + jnp.dot(
                    mixed_in[l, pl.ds(i * N_DP, N_DP)].reshape(N_DP * ROWS, WIDTH), w_out[l, i], preferred_element_type=F32
                )
            osum[l] = out_part.reshape(N_Z, ROWS, FEATS).astype(BF16)
            for _, p in z_peers:
                send(osum.at[l, p], osum_in.at[l, z], l, 3, {"tp": p * N_X + x})
            osum_in[l, z] = osum[l, z]
        with jax.named_scope("wait_sum"):
            wait_bytes(osum_in.at[l, pl.ds(0, N_Z - 1)], recv_sem.at[l, 3])
        with jax.named_scope("send_rows"):
            own = first[me_t] if l == 0 else rows[0]
            new = own.astype(F32) + jnp.sum(osum_in[l].astype(F32), axis=0)
            rows[l] = new.astype(BF16)
            target = stream_mid if l == 0 else stream_out
            for dz, p in z_peers:
                send(rows.at[l], target.at[me_t], l, 4, {"tp": p * N_X + x}, sem=ring_sem.at[l, dz])
            for p in x_peers:
                send(rows.at[l], target.at[me_t], l, 4, {"tp": z * N_X + p})
            target[me_t] = rows[l]
        with jax.named_scope("wait_rows"):
            for dz in Z_STEPS[::-1]:
                src = (z + N_Z - dz) % N_Z * N_X + x
                wait_bytes(target.at[0], ring_sem.at[l, dz])
                for p in x_peers:
                    send(target.at[src], target.at[src], l, 4, {"tp": z * N_X + p})
            wait_bytes(target.at[pl.ds(0, N_TP - N_Z)], recv_sem.at[l, 4])

    with jax.named_scope("drain"):
        for l in range(BLOCKS):
            wait_bytes(part.at[l, pl.ds(0, N_DP - 1)], send_sem.at[l, 0])
            wait_bytes(sq_in.at[l, pl.ds(0, N_DP - 1)], send_sem.at[l, 1])
            wait_bytes(mixed_in.at[l, pl.ds(0, len(slab_peers))], send_sem.at[l, 2])
            wait_bytes(osum.at[l, pl.ds(0, N_Z - 1)], send_sem.at[l, 3])
            wait_bytes(stream_mid.at[pl.ds(0, N_TP - 1)], send_sem.at[l, 4])
            wait_bytes(w_out.at[l, pl.ds(0, N_X - 1)], send_sem.at[l, 5])


def put(stream_in, state_in, stream_out, state_out, sem):
    copies = [
        pltpu.make_async_copy(state_in, state_out, sem.at[0]),
        pltpu.make_async_copy(stream_in, stream_out, sem.at[1]),
    ]
    for c in copies:
        c.start()
    for c in copies:
        c.wait()


def body(
    stream, history, input_norm_gain, query_weight, key_weight, value_weight, gate_weight, adapter_down_weight,
    decay_up_weight, rate_up_weight, decay_offset, head_norm_gain, output_weight, recurrent_state,
):
    state = recurrent_state.reshape(BLOCKS, SEQS, 2, HEAD // 2, WIDTH).transpose(0, 1, 3, 2, 4)
    state = state.reshape(BLOCKS, PAIRS, WIDTH)
    vmem, hbm = pl.BlockSpec(memory_space=pltpu.VMEM), pl.BlockSpec(memory_space=pltpu.HBM)
    stream_shape, state_shape = (N_TP, ROWS, FEATS), (BLOCKS, PAIRS, WIDTH)
    new_stream, new_state = pl.pallas_call(
        kernel,
        out_shape=(pltpu.VMEM(stream_shape, BF16), pltpu.VMEM(state_shape, F32)),
        in_specs=[hbm] * 14,
        out_specs=(vmem, vmem),
        scratch_shapes=[
            pltpu.SMEM((SEQS,), jnp.int32),
            pltpu.VMEM((BLOCKS, FEATS), F32),
            pltpu.VMEM((BLOCKS, WIDTH), F32),
            pltpu.VMEM((BLOCKS, WIDTH), F32),
            pltpu.VMEM(stream_shape, BF16),
            pltpu.VMEM((BLOCKS, FEATS, WIDE), BF16),
            pltpu.VMEM((BLOCKS, 2 * ADAPTER_RANK, 2 * WIDTH), F32),
            pltpu.VMEM((BLOCKS, N_X, WIDTH, FEATS), BF16),
            pltpu.VMEM(state_shape, F32),
            pltpu.VMEM((BLOCKS, N_DP, SEQS, WIDE), BF16),
            pltpu.VMEM((BLOCKS, N_DP, SEQS, WIDE), BF16),
            pltpu.VMEM((BLOCKS, 1, BATCH), F32),
            pltpu.VMEM((BLOCKS, N_DP, 1, BATCH), F32),
            pltpu.VMEM((BLOCKS, N_X, ROWS, WIDTH), BF16),
            pltpu.VMEM((BLOCKS, N_X * N_DP, ROWS, WIDTH), BF16),
            pltpu.VMEM((BLOCKS, N_Z, ROWS, FEATS), BF16),
            pltpu.VMEM((BLOCKS, N_Z, ROWS, FEATS), BF16),
            pltpu.VMEM((BLOCKS, ROWS, FEATS), BF16),
            pltpu.VMEM(stream_shape, BF16),
            pltpu.SemaphoreType.DMA((BLOCKS, 9)),
            pltpu.SemaphoreType.DMA((5,)),
            pltpu.SemaphoreType.DMA((BLOCKS, 6)),
            pltpu.SemaphoreType.DMA((BLOCKS, 6)),
            pltpu.SemaphoreType.DMA((BLOCKS, N_Z)),
        ],
        compiler_params=pltpu.CompilerParams(
            collective_id=0, has_side_effects=True, vmem_limit_bytes=64684032
        ),
        name="two_blocks",
    )(
        history, input_norm_gain, decay_offset, head_norm_gain, stream.reshape(stream_shape),
        query_weight, key_weight, value_weight, gate_weight, adapter_down_weight,
        decay_up_weight, rate_up_weight, output_weight, state,
    )
    new_stream, new_state = pl.pallas_call(
        put,
        out_shape=(jax.ShapeDtypeStruct(stream_shape, BF16), jax.ShapeDtypeStruct(state_shape, F32)),
        in_specs=[vmem, vmem],
        out_specs=(hbm, hbm),
        scratch_shapes=[pltpu.SemaphoreType.DMA((2,))],
        compiler_params=pltpu.CompilerParams(vmem_limit_bytes=2**20),
        name="put",
    )(new_stream, new_state)
    new_state = new_state.reshape(BLOCKS, SEQS, HEAD // 2, 2, WIDTH).transpose(0, 1, 3, 2, 4)
    return new_stream.reshape(BATCH, FEATS), new_state.reshape(BLOCKS, SEQS, 2, HEAD * HEAD)


def solution(mesh):
    placed = (
        P(None, "dp"), P("dp"), P(None, "dp"),
        P(None, "dp", "tp"), P(None, "dp", "tp"), P(None, "dp", "tp"), P(None, "dp", "tp"),
        P(None, "dp", None), P(None, None, "tp"), P(None, None, "tp"), P(None, "tp"), P(None, "tp"),
        P(None, "tp", "dp"), P(None, "dp", "tp", None),
    )
    return jax.shard_map(
        body,
        mesh=mesh,
        in_specs=placed,
        out_specs=(P(None, "dp"), P(None, "dp", "tp", None)),
        check_vma=False,
    )
```

```python
import jax
import jax.numpy as jnp
from jax import lax
from jax.experimental import pallas as pl
from jax.experimental.pallas import tpu as pltpu
from jax.sharding import PartitionSpec as P

MODEL_WIDTH = 4096
HEAD = 64
ADAPTER_RANK = 64
SPAN = 64
BLOCKS = 2
NORM_EPS = 0.25
GROUP_EPS = 0.25

N_Y, N_CORE, N_Z, N_X = 4, 2, 8, 4
N_DP, N_TP = N_Y * N_CORE, N_Z * N_X
BATCH = 256
SEQS = BATCH // N_DP
ROWS = BATCH // N_TP
FEATS = MODEL_WIDTH // N_DP
WIDTH = MODEL_WIDTH // N_TP
PAIRS = SEQS * HEAD
WIDE = 4 * WIDTH + 2 * ADAPTER_RANK

F32, BF16 = jnp.float32, jnp.bfloat16
MESH = pl.DeviceIdType.MESH

def hops(step, size):
    return min(step, size - step)


DP_STEPS = [(dy, dc) for dy in (2, 1, 3) for dc in (0, 1)] + [(0, 1)]
Y_STEPS = [2, 1, 3]
Z_STEPS = [4, 3, 5, 2, 6, 1, 7]
X_STEPS = [2, 1, 3]
SLAB_STEPS = sorted(
    [(dx, dy, dc) for dx in range(N_X) for dy in range(N_Y) for dc in range(N_CORE) if (dx, dy, dc) != (0, 0, 0)],
    key=lambda s: -(hops(s[0], N_X) + hops(s[1], N_Y)),
)
FORWARD = {1: (2, 1, 3), 7: (2, 1, 3), 2: (2, 1, 3), 6: (2, 1, 3), 3: (1, 3), 5: (1, 3)}
ROW_STEPS = [(3, 0), (5, 0), (2, 0), (6, 0), (4, 2), (4, 1), (4, 3), (3, 2), (5, 2), (4, 0), (1, 0), (7, 0)]
ROW_STEPS += [(0, 2), (0, 1), (0, 3)]


def stable_sigmoid(x):
    e = jnp.exp(-jnp.abs(x))
    return jnp.where(x >= 0, 1.0, e) / (1.0 + e)


def iota(shape, dim):
    return lax.broadcasted_iota(jnp.int32, shape, dim)


def kernel(
    hist_in, gain_in, decay_off_in, head_gain_in, stream_in, qw, kw, vw, gw, aw, du, ru, ow, state_in,
    stream_out, state_out,
    hist, gains, decay_off, head_gain, first, w_first, w_second, low_raw, w_low, w_out, state,
    part0, part0_in, part1, part1_in, sq0, sq0_in, sq1, sq1_in, mixed, mixed_in, osum, osum_in, rows, stream_mid,
    load_sem, misc_sem, send_sem, recv_sem, ring_sem,
):
    me_t, me_d = lax.axis_index("tp"), lax.axis_index("dp")
    z, x = me_t // N_X, me_t % N_X
    y, core = me_d // N_CORE, me_d % N_CORE
    dp_peers = [((y + dy) % N_Y) * N_CORE + (core + dc) % N_CORE for dy, dc in DP_STEPS]
    y_peers = [(y + dy) % N_Y for dy in Y_STEPS]
    z_peers = [(dz, (z + dz) % N_Z) for dz in Z_STEPS]
    x_peers = [(x + dx) % N_X for dx in X_STEPS]
    slab_peers = [
        ((x + dx) % N_X, ((y + dy) % N_Y) * N_CORE + (core + dc) % N_CORE) for dx, dy, dc in SLAB_STEPS
    ]
    partner = y * N_CORE + (core + 1) % N_CORE

    def start(src, dst, sem):
        c = pltpu.make_async_copy(src, dst, sem)
        c.start()
        return c

    def load_weights(l, dst):
        return [
            start(w.at[l], dst.at[:, pl.ds(i * WIDTH, WIDTH)], load_sem.at[l, i])
            for i, w in enumerate((qw, kw, vw, gw, aw))
        ]

    def load_small(l):
        return [
            start(du.at[l], low_raw.at[l, 0], load_sem.at[l, 5]),
            start(ru.at[l], low_raw.at[l, 1], load_sem.at[l, 6]),
            start(ow.at[l], w_out.at[l, x], load_sem.at[l, 7]),
        ]

    def load_state(l):
        return start(state_in.at[l], state.at[l], load_sem.at[l, 8])

    first_loads = [start(stream_in, first, misc_sem.at[0]), start(gain_in, gains.at[core], misc_sem.at[1])]
    weight_loads = load_weights(0, w_first)

    barrier = pltpu.get_barrier_semaphore()
    for px, pd in slab_peers:
        pl.semaphore_signal(barrier, inc=1, device_id={"tp": z * N_X + px, "dp": pd}, device_id_type=MESH)
    for _, p in z_peers:
        pl.semaphore_signal(barrier, inc=1, device_id={"tp": p * N_X + x}, device_id_type=MESH)

    def send(src, dst, l, s, peer, sem=None):
        pltpu.make_async_remote_copy(
            src_ref=src, dst_ref=dst, send_sem=send_sem.at[l, s],
            recv_sem=recv_sem.at[l, s] if sem is None else sem,
            device_id=peer, device_id_type=MESH,
        ).start()

    def wait_bytes(ref, sem):
        pltpu.make_async_copy(ref, ref, sem).wait()

    def halves(v):
        hi = v.astype(BF16)
        return hi, (v - hi.astype(F32)).astype(BF16)

    def split_dot(v, m):
        hi, lo = halves(v)
        return jnp.dot(hi, m, preferred_element_type=F32) + jnp.dot(lo, m, preferred_element_type=F32)

    def same(shape, group_a, group_b):
        return (group_a(iota(shape, 0)) == group_b(iota(shape, 1))).astype(F32).astype(BF16)

    eye = iota((128, 128), 0) == iota((128, 128), 1)

    def squares(xs):
        col = sum(jnp.sum(v * v, axis=1, keepdims=True) for v in xs)
        return [
            jnp.sum(jnp.where(eye, col[i : i + 128], 0.0), axis=0, keepdims=True) for i in range(0, col.shape[0], 128)
        ]

    for l in range(BLOCKS):
        with jax.named_scope("project"):
            if l == 0:
                for c in first_loads:
                    c.wait()
                xs = [first[...].astype(F32).reshape(BATCH, FEATS)]
                scaled = (xs[0] * gains[core, pl.ds(0, 1), :]).astype(BF16)
                for c in weight_loads:
                    c.wait()
                product = jnp.dot(scaled, w_first[...], preferred_element_type=F32)
                part0[...] = product.astype(BF16).reshape(N_DP, SEQS, WIDE)
                small_loads = load_small(0) + [
                    start(hist_in, hist, misc_sem.at[2]),
                    start(decay_off_in, decay_off, misc_sem.at[3]),
                    start(head_gain_in, head_gain, misc_sem.at[4]),
                ]
                state_load = load_state(0)
            else:
                half = N_TP // N_CORE
                xs = [
                    stream_mid[pl.ds(c * half, half)].astype(F32).reshape(BATCH // N_CORE, FEATS)
                    for c in range(N_CORE)
                ]
                product = sum(
                    jnp.dot(
                        (xs[c] * gains[c, pl.ds(1, 1), :]).astype(BF16), w_second[c], preferred_element_type=F32
                    )
                    for c in range(N_CORE)
                )
                part1[...] = product.astype(BF16).reshape(N_Y, SEQS, WIDE)
        with jax.named_scope("barrier"):
            if l == 0:
                pl.semaphore_wait(barrier, len(slab_peers) + len(z_peers))
        with jax.named_scope("send_part"):
            if l == 0:
                for p in dp_peers:
                    send(part0.at[p], part0_in.at[me_d], l, 0, {"dp": p})
                for i, v in enumerate(squares(xs)):
                    sq0[:, pl.ds(i * 128, 128)] = v
                for p in dp_peers:
                    send(sq0, sq0_in.at[me_d], l, 1, {"dp": p})
                part0_in[me_d] = part0[me_d]
                sq0_in[me_d] = sq0[...]
            else:
                for p in y_peers:
                    send(part1.at[p], part1_in.at[y], l, 0, {"dp": p * N_CORE + core})
                sq1[...] = squares(xs)[0]
                for p in y_peers:
                    send(sq1, sq1_in.at[y], l, 1, {"dp": p * N_CORE + core})
                part1_in[y] = part1[y]
                sq1_in[y] = sq1[...]
            for p in x_peers:
                send(ow.at[l], w_out.at[l, x], l, 5, {"tp": z * N_X + p})
            if l == 0:
                send(gains.at[core], gains.at[core], l, 6, {"dp": partner})
                next_weights = load_weights(1, w_second.at[core])
            for c in small_loads:
                c.wait()
            none = jnp.zeros((ADAPTER_RANK, WIDTH), F32)
            up_hi, up_lo = halves(jnp.concatenate([
                jnp.concatenate([low_raw[l, 0], none], axis=1), jnp.concatenate([none, low_raw[l, 1]], axis=1)
            ], axis=0))
            w_low[l] = jnp.concatenate([up_hi, up_hi, up_lo], axis=0)
            if l == 0:
                low_lane = iota((SEQS, WIDTH), 1) < HEAD
                head = lambda i: i % WIDTH // HEAD
                seg = same((2 * WIDTH, WIDTH), head, head)
                fold = same((2 * WIDTH, 2 * WIDTH), lambda i: i // HEAD, lambda i: i // WIDTH * 2 + i % 2)
                spread = same((WIDTH, WIDTH), lambda i: i % 2, head)
                r_i, l_i = iota((HEAD, WIDTH), 0), iota((HEAD, WIDTH), 1)
                pick = ((l_i // HEAD == r_i % 2) & ((l_i % HEAD) // 2 == r_i // 2)).astype(F32)
                even_row = (iota((SEQS, 8, WIDTH), 1) % 2) == 0
                pos = jnp.zeros((SEQS, WIDTH), F32)
                seq_i = iota((SEQS, WIDTH), 0)
                for i in range(SEQS):
                    pos = jnp.where(seq_i == i, 0.5 + ((hist[i] // SPAN) % 3).astype(F32), pos)
            state_load.wait()
        with jax.named_scope("wait_part"):
            part_in, sq_in = (part0_in, sq0_in) if l == 0 else (part1_in, sq1_in)
            count, place = (N_DP, me_d) if l == 0 else (N_Y, y)
            wait_bytes(sq_in.at[pl.ds(0, count - 1)], recv_sem.at[l, 1])
            sq_all = sq_in[0]
            for d in range(1, count):
                sq_all = sq_all + sq_in[d]
            shape = (SEQS, count * SEQS)
            mine = iota(shape, 1) == iota(shape, 0) + place * SEQS
            own_sq = jnp.sum(jnp.where(mine, sq_all, 0.0), axis=1, keepdims=True)
            inv = lax.rsqrt(own_sq / MODEL_WIDTH + NORM_EPS)
            wait_bytes(part_in.at[pl.ds(0, count - 1)], recv_sem.at[l, 0])
        with jax.named_scope("recur"):
            total = part_in[0].astype(F32)
            for d in range(1, count):
                total = total + part_in[d].astype(F32)
            total = total * inv
            query, key, value, gate, low = [total[:, i * WIDTH : (i + 1) * WIDTH] for i in range(5)]

            def seg_dot(v):
                return jnp.dot(jnp.concatenate(halves(v), axis=1), seg, preferred_element_type=F32)

            def per_row(v):
                r = pltpu.roll(v, HEAD, 1)
                t0, t1 = jnp.where(low_lane, v, r), jnp.where(low_lane, r, v)
                return jnp.where(even_row, t0[:, None, :], t1[:, None, :])

            low_hi, low_lo = halves(jnp.where(low_lane, jnp.tanh(low), low))
            up = jnp.dot(
                jnp.concatenate([low_hi, low_lo, low_hi], axis=1), w_low[l], preferred_element_type=F32
            )
            decay = jnp.exp(
                -(stable_sigmoid(decay_off[pl.ds(l, 1), :] + up[:, :WIDTH]) * 0.6065306597126334) * pos
            )
            learn = stable_sigmoid(up[:, WIDTH:])
            sums = seg_dot(jnp.concatenate([key * key, key * learn * query, key * query], axis=0))
            key_inv = lax.rsqrt(sums[:SEQS] + 1.0)
            key_unit = key * key_inv
            key_rate = key_unit * learn
            rate_query, key_query = sums[SEQS : 2 * SEQS] * key_inv, sums[2 * SEQS :]

            held = state[l].reshape(SEQS, HEAD // 8, 8, WIDTH)
            prods = jnp.concatenate([
                (held * per_row(v)[:, None]).reshape(PAIRS, WIDTH) for v in (key_unit, decay * query)
            ], axis=1)
            folded = split_dot(prods, fold).reshape(SEQS, HEAD, 2 * WIDTH)
            state_key = jnp.sum(folded[:, :, :WIDTH] * pick[None], axis=1)
            state_query = jnp.sum(folded[:, :, WIDTH:] * pick[None], axis=1)
            readout = state_query - state_key * rate_query + value * key_query
            centred = readout - seg_dot(readout) * (1.0 / HEAD)
            var = seg_dot(centred * centred) * (1.0 / HEAD)
            normed = centred * lax.rsqrt(var + GROUP_EPS) * head_gain[pl.ds(l, 1), :]
            own_mixed = (normed * stable_sigmoid(gate)).astype(BF16)
        with jax.named_scope("send_mixed"):
            mixed[l] = own_mixed.reshape(N_X, ROWS, WIDTH)
            for px, pd in slab_peers:
                send(mixed.at[l, px], mixed_in.at[l, x * N_DP + me_d], l, 2, {"tp": z * N_X + px, "dp": pd})
            mixed_in[l, x * N_DP + me_d] = mixed[l, x]
        with jax.named_scope("update"):
            if l == 0:
                for c in next_weights:
                    c.wait()
                send(w_second.at[core], w_second.at[core], l, 7, {"dp": partner})
                small_loads = load_small(1)
                state_load = load_state(1)

            def outer(v):
                return split_dot((v[:, None, :] * pick[None]).reshape(PAIRS, WIDTH), spread).reshape(
                    SEQS, HEAD // 8, 8, WIDTH
                )

            state_out[l] = (
                held * per_row(decay)[:, None]
                - outer(state_key) * per_row(key_rate)[:, None]
                + outer(value) * per_row(key)[:, None]
            ).reshape(PAIRS, WIDTH)
        with jax.named_scope("wait_mixed"):
            wait_bytes(w_out.at[l, pl.ds(0, N_X - 1)], recv_sem.at[l, 5])
            wait_bytes(mixed_in.at[l, pl.ds(0, len(slab_peers))], recv_sem.at[l, 2])
        with jax.named_scope("output"):
            out_part = jnp.zeros((N_DP * ROWS, FEATS), F32)
            for i in range(N_X):
                out_part = out_part + jnp.dot(
                    mixed_in[l, pl.ds(i * N_DP, N_DP)].reshape(N_DP * ROWS, WIDTH), w_out[l, i],
                    preferred_element_type=F32,
                )
            osum[l] = out_part.reshape(N_Z, ROWS, FEATS).astype(BF16)
            for _, p in z_peers:
                send(osum.at[l, p], osum_in.at[l, z], l, 3, {"tp": p * N_X + x})
            osum_in[l, z] = osum[l, z]
        with jax.named_scope("wait_sum"):
            wait_bytes(osum_in.at[l, pl.ds(0, N_Z - 1)], recv_sem.at[l, 3])
        with jax.named_scope("send_rows"):
            own = first[me_t] if l == 0 else rows[0]
            new = own.astype(F32) + jnp.sum(osum_in[l].astype(F32), axis=0)
            rows[l] = new.astype(BF16)
            if l == 0:
                target, row_d = stream_mid, y * N_CORE + z % N_CORE
                place = lambda pz, c: c * (N_TP // N_CORE) + pz // N_CORE * N_X + x
            else:
                target, row_d = stream_out, me_d
                place = lambda pz, c: pz * N_X + x
            here = place(z, core)
            for dz, dx in ROW_STEPS:
                send(
                    rows.at[l], target.at[here], l, 4,
                    {"tp": (z + dz) % N_Z * N_X + (x + dx) % N_X, "dp": row_d},
                    sem=ring_sem.at[l, dz, core] if dx == 0 and dz in FORWARD else None,
                )

            def pass_on(dz, c):
                there = place((z + N_Z - dz) % N_Z, c)
                wait_bytes(target.at[0], ring_sem.at[l, dz, c])
                for dx in FORWARD[dz]:
                    pltpu.make_async_remote_copy(
                        src_ref=target.at[there], dst_ref=target.at[there], send_sem=send_sem.at[1, 6 + l],
                        recv_sem=recv_sem.at[l, 4], device_id={"tp": z * N_X + (x + dx) % N_X}, device_id_type=MESH,
                    ).start()

        with jax.named_scope("wait_rows"):
            if l == 0:
                even = (z + core) % 2 == 0

                @pl.when(even)
                def _():
                    target[here] = rows[l]
                    for dz in (2, 6):
                        for c in range(N_CORE):
                            pass_on(dz, c)
                    wait_bytes(target.at[pl.ds(0, 27)], recv_sem.at[l, 4])

                @pl.when(jnp.logical_not(even))
                def _():
                    pltpu.make_async_remote_copy(
                        src_ref=rows.at[l], dst_ref=target.at[here], send_sem=send_sem.at[1, 8],
                        recv_sem=recv_sem.at[l, 4], device_id={"dp": partner}, device_id_type=MESH,
                    ).start()
                    for dz in (1, 7, 3, 5):
                        for c in range(N_CORE):
                            pass_on(dz, c)
                    wait_bytes(target.at[pl.ds(0, 24)], recv_sem.at[l, 4])

                wait_bytes(gains.at[0], recv_sem.at[l, 6])
                wait_bytes(w_second.at[0], recv_sem.at[l, 7])
            else:
                target[here] = rows[l]
                for dz in (1, 7, 2, 6, 3, 5):
                    pass_on(dz, core)
                wait_bytes(target.at[pl.ds(0, 25)], recv_sem.at[l, 4])

    with jax.named_scope("drain"):
        wait_bytes(part0.at[pl.ds(0, N_DP - 1)], send_sem.at[0, 0])
        wait_bytes(sq0_in.at[pl.ds(0, N_DP - 1)], send_sem.at[0, 1])
        wait_bytes(part1.at[pl.ds(0, N_Y - 1)], send_sem.at[1, 0])
        wait_bytes(sq1_in.at[pl.ds(0, N_Y - 1)], send_sem.at[1, 1])
        wait_bytes(gains.at[0], send_sem.at[0, 6])
        wait_bytes(w_second.at[0], send_sem.at[0, 7])
        for l in range(BLOCKS):
            wait_bytes(mixed_in.at[l, pl.ds(0, len(slab_peers))], send_sem.at[l, 2])
            wait_bytes(osum.at[l, pl.ds(0, N_Z - 1)], send_sem.at[l, 3])
            wait_bytes(stream_mid.at[pl.ds(0, len(ROW_STEPS))], send_sem.at[l, 4])
            wait_bytes(w_out.at[l, pl.ds(0, N_X - 1)], send_sem.at[l, 5])
        wait_bytes(stream_mid.at[pl.ds(0, 16)], send_sem.at[1, 7])

        @pl.when((z + core) % 2 == 0)
        def _():
            wait_bytes(stream_mid.at[pl.ds(0, 12)], send_sem.at[1, 6])

        @pl.when((z + core) % 2 != 0)
        def _():
            wait_bytes(stream_mid.at[pl.ds(0, 20)], send_sem.at[1, 6])
            wait_bytes(stream_mid.at[0], send_sem.at[1, 8])


def put(stream_in, state_in, stream_out, state_out, sem):
    copies = [
        pltpu.make_async_copy(state_in, state_out, sem.at[0]),
        pltpu.make_async_copy(stream_in, stream_out, sem.at[1]),
    ]
    for c in copies:
        c.start()
    for c in copies:
        c.wait()


def body(
    stream, history, input_norm_gain, query_weight, key_weight, value_weight, gate_weight, adapter_down_weight,
    decay_up_weight, rate_up_weight, decay_offset, head_norm_gain, output_weight, recurrent_state,
):
    state = recurrent_state.reshape(BLOCKS, SEQS, 2, HEAD // 2, WIDTH).transpose(0, 1, 3, 2, 4)
    state = state.reshape(BLOCKS, PAIRS, WIDTH)
    vmem, hbm = pl.BlockSpec(memory_space=pltpu.VMEM), pl.BlockSpec(memory_space=pltpu.HBM)
    stream_shape, state_shape = (N_TP, ROWS, FEATS), (BLOCKS, PAIRS, WIDTH)
    new_stream, new_state = pl.pallas_call(
        kernel,
        out_shape=(pltpu.VMEM(stream_shape, BF16), pltpu.VMEM(state_shape, F32)),
        in_specs=[hbm] * 14,
        out_specs=(vmem, vmem),
        scratch_shapes=[
            pltpu.SMEM((SEQS,), jnp.int32),
            pltpu.VMEM((N_CORE, BLOCKS, FEATS), F32),
            pltpu.VMEM((BLOCKS, WIDTH), F32),
            pltpu.VMEM((BLOCKS, WIDTH), F32),
            pltpu.VMEM(stream_shape, BF16),
            pltpu.VMEM((FEATS, WIDE), BF16),
            pltpu.VMEM((N_CORE, FEATS, WIDE), BF16),
            pltpu.VMEM((BLOCKS, 2, ADAPTER_RANK, WIDTH), F32),
            pltpu.VMEM((BLOCKS, 6 * ADAPTER_RANK, 2 * WIDTH), BF16),
            pltpu.VMEM((BLOCKS, N_X, WIDTH, FEATS), BF16),
            pltpu.VMEM(state_shape, F32),
            pltpu.VMEM((N_DP, SEQS, WIDE), BF16),
            pltpu.VMEM((N_DP, SEQS, WIDE), BF16),
            pltpu.VMEM((N_Y, SEQS, WIDE), BF16),
            pltpu.VMEM((N_Y, SEQS, WIDE), BF16),
            pltpu.VMEM((1, BATCH), F32),
            pltpu.VMEM((N_DP, 1, BATCH), F32),
            pltpu.VMEM((1, BATCH // N_CORE), F32),
            pltpu.VMEM((N_Y, 1, BATCH // N_CORE), F32),
            pltpu.VMEM((BLOCKS, N_X, ROWS, WIDTH), BF16),
            pltpu.VMEM((BLOCKS, N_X * N_DP, ROWS, WIDTH), BF16),
            pltpu.VMEM((BLOCKS, N_Z, ROWS, FEATS), BF16),
            pltpu.VMEM((BLOCKS, N_Z, ROWS, FEATS), BF16),
            pltpu.VMEM((BLOCKS, ROWS, FEATS), BF16),
            pltpu.VMEM(stream_shape, BF16),
            pltpu.SemaphoreType.DMA((BLOCKS, 9)),
            pltpu.SemaphoreType.DMA((5,)),
            pltpu.SemaphoreType.DMA((BLOCKS, 9)),
            pltpu.SemaphoreType.DMA((BLOCKS, 8)),
            pltpu.SemaphoreType.DMA((BLOCKS, N_Z, N_CORE)),
        ],
        compiler_params=pltpu.CompilerParams(
            collective_id=0, has_side_effects=True, vmem_limit_bytes=64684032
        ),
        name="two_blocks",
    )(
        history, input_norm_gain, decay_offset, head_norm_gain, stream.reshape(stream_shape),
        query_weight, key_weight, value_weight, gate_weight, adapter_down_weight,
        decay_up_weight, rate_up_weight, output_weight, state,
    )
    new_stream, new_state = pl.pallas_call(
        put,
        out_shape=(jax.ShapeDtypeStruct(stream_shape, BF16), jax.ShapeDtypeStruct(state_shape, F32)),
        in_specs=[vmem, vmem],
        out_specs=(hbm, hbm),
        scratch_shapes=[pltpu.SemaphoreType.DMA((2,))],
        compiler_params=pltpu.CompilerParams(vmem_limit_bytes=2**20),
        name="put",
    )(new_stream, new_state)
    new_state = new_state.reshape(BLOCKS, SEQS, HEAD // 2, 2, WIDTH).transpose(0, 1, 3, 2, 4)
    return new_stream.reshape(BATCH, FEATS), new_state.reshape(BLOCKS, SEQS, 2, HEAD * HEAD)


def solution(mesh):
    placed = (
        P(None, "dp"), P("dp"), P(None, "dp"),
        P(None, "dp", "tp"), P(None, "dp", "tp"), P(None, "dp", "tp"), P(None, "dp", "tp"),
        P(None, "dp", None), P(None, None, "tp"), P(None, None, "tp"), P(None, "tp"), P(None, "tp"),
        P(None, "tp", "dp"), P(None, "dp", "tp", None),
    )
    return jax.shard_map(
        body,
        mesh=mesh,
        in_specs=placed,
        out_specs=(P(None, "dp"), P(None, "dp", "tp", None)),
        check_vma=False,
    )
```
